128 devices in a mesh: fs: 32 (over z, y, core), tp: 4 (over x).
Axes of the slice: x: 4, y: 4, z: 4, core: 2. Of those that a mesh axis runs over, the one named last changes fastest.
Arguments:
- tokens: bfloat16 [49152, 2048], P('fs', 'tp'), may hold values from -6 to 6
- norm_gain: float32 [2048], P('fs'), may hold values from 0.1 to 1.9
- up_weight: float32 [2048, 8192], P('fs', 'tp'), may hold values from -0.125 to 0.125
- down_weight: float32 [2048, 8192], P('fs', 'tp'), may hold values from -0.0625 to 0.0625
Outputs:
- up_matrix: bfloat16 [2048, 8192], P(None, 'tp')
- down_matrix: bfloat16 [2048, 8192], P(None, 'tp')
- mixed: bfloat16 [49152, 2048], P('fs', 'tp')
The draws below stay inside these ranges and needn't reach their ends.
All inputs are finite; a program needn't handle non-finite values.
Results may differ from the reference program's by a relative error of at most 0.0095.
Values may be sent and summed in bfloat16 or wider, within the bound.
A program may use at most 128 MiB of HBM per device.

```python
import jax
import jax.numpy as jnp
from jax import lax

D = 2048
FF = 8192
TOKENS = 49152
N_TP = 4


def levels(rng, shape, pieces, smallest, high):
    factor_of, own = 1.0, jax.random.fold_in(rng, 6)
    for dim, parts in pieces:
        draws = jnp.exp(jax.random.uniform(jax.random.fold_in(own, dim), (parts,), jnp.float32, smallest / len(pieces), high / len(pieces)))
        factor_of = factor_of * jnp.repeat(draws, shape[dim] // parts).reshape([-1 if axis == dim else 1 for axis in range(len(shape))])
    return factor_of


def bell_draw(stream_key, dims, deviation, most, pieces=(), kind=jnp.bfloat16):
    loudness = levels(stream_key, dims, pieces, -0.22, 0.18) if pieces else 1.0
    drawn = jax.random.normal(stream_key, dims, jnp.float32) * deviation * loudness
    return jnp.minimum(jnp.maximum(drawn, -most), most).astype(kind)


def setup_inputs(seed: int = 0) -> dict:
    arg_keys = jax.random.split(jax.random.key(seed), 5)
    tokens = bell_draw(arg_keys[0], (TOKENS, D), 1.0, 6.0, ((0, 32), (1, 4)))
    norm_gain = jnp.clip(1.0 + 0.18 * jax.random.normal(arg_keys[1], (D,), jnp.float32), 0.1, 1.9)
    up_weight = bell_draw(arg_keys[2], (D, FF), D ** -0.5, 0.125, ((0, 32), (1, 4)), jnp.float32)
    down_weight = bell_draw(arg_keys[3], (D, FF), FF ** -0.5, 0.0625, ((0, 32), (1, 4)), jnp.float32)
    return dict(tokens=tokens, norm_gain=norm_gain, up_weight=up_weight, down_weight=down_weight)


epsilon = 1e-06

def reference(tokens, norm_gain, up_weight, down_weight):
    up_matrix = (norm_gain[:, None] * up_weight).astype(jnp.bfloat16)
    down_matrix = down_weight.astype(jnp.bfloat16)
    widened = tokens.astype(jnp.float32)
    normed = (widened * lax.rsqrt(lax.optimization_barrier(jnp.mean(widened * widened, axis=-1, keepdims=True)) + epsilon)).astype(jnp.bfloat16)
    width = FF // N_TP
    mixed_sum = jnp.zeros((tokens.shape[0], tokens.shape[1]), jnp.float32)
    for group_index in range(N_TP):
        up_block = up_matrix[:, group_index * width:(group_index + 1) * width]
        down_block = down_matrix[:, group_index * width:(group_index + 1) * width]
        up_values = jnp.dot(normed, up_block, preferred_element_type=jnp.float32)
        hidden = jnp.square(jax.nn.relu(up_values)).astype(jnp.bfloat16)
        partial_value = lax.dot_general(hidden, down_block, (((1,), (1,)), ((), ())), preferred_element_type=jnp.float32)
        mixed_sum = mixed_sum + partial_value.astype(jnp.bfloat16).astype(jnp.float32)
    return (up_matrix, down_matrix, mixed_sum.astype(jnp.bfloat16))
```

```python
import functools

import jax
import jax.numpy as jnp
from jax import lax
from jax.experimental import pallas as pl
from jax.experimental.pallas import tpu as pltpu
from jax.sharding import PartitionSpec as P

epsilon = 1e-06
RING = 4
HALF = 32
PIECE = 128
CHUNK = 256
MESH = pl.DeviceIdType.MESH
F32, BF16 = jnp.float32, jnp.bfloat16


def onward(at, first, second, half):
    links = []
    if at[second] == 0:
        if at[first] == 0:
            links += [(first, 1), (first, -1)]
        elif at[first] == 1 and half == 0:
            links += [(first, 1)]
        elif at[first] == -1 and half == 1:
            links += [(first, -1)]
        links += [(second, 1), (second, -1)]
    elif at[second] == 1 and half == 0:
        links += [(second, 1)]
    elif at[second] == -1 and half == 1:
        links += [(second, -1)]
    return links


def weight_plan():
    links = [(axis, sign) for axis in "yz" for sign in (1, -1)]
    queues = {link: [] for link in links}

    def offer(unit, slot):
        matrix, z, y, half = unit
        first, second = ("y", "z") if matrix == 0 else ("z", "y")
        for link in onward({"z": z, "y": y}, first, second, half):
            queues[link].append((0 if link[0] == first else 1, slot, unit))

    for half in (0, 1):
        for matrix in (0, 1):
            offer((matrix, 0, 0, half), 0)
    slots, landed = [], {}
    while any(queues.values()) or any(landed.values()):
        now = len(slots)
        for unit in landed.pop(now - 2, []):
            offer(unit, now)
        leaving = []
        for link in links:
            if queues[link]:
                choice = min(queues[link], key=lambda entry: entry[:2])
                queues[link].remove(choice)
                leaving.append((link, choice[2]))
        landed[now] = []
        for (axis, sign), (matrix, z, y, half) in leaving:
            landed[now].append((matrix, z + sign * (axis == "z"), y + sign * (axis == "y"), half))
        slots.append(leaving)
        if len(slots) > 100:
            raise ValueError("plan")
    while slots and not slots[-1]:
        slots.pop()
    return slots


def token_plan(pieces):
    own = {1: list(range(pieces)), -1: list(range(pieces))}
    passing = {1: [], -1: []}
    slots, landed = [], {}
    while own[1] or own[-1] or passing[1] or passing[-1] or any(landed.values()):
        now = len(slots)
        for sign, hops, piece in landed.pop(now - 2, []):
            if hops == 1 and (piece % 2 == 0) == (sign == 1):
                passing[sign].append(piece)
        leaving = []
        for sign in (1, -1):
            if passing[sign]:
                leaving.append((sign, 1, passing[sign].pop(0)))
            elif own[sign]:
                leaving.append((sign, 0, own[sign].pop(0)))
        landed[now] = [(sign, hops + 1, piece) for sign, hops, piece in leaving]
        slots.append(leaving)
    while slots and not slots[-1]:
        slots.pop()
    return slots


def place():
    fs, x = lax.axis_index("fs"), lax.axis_index("tp")
    core, chip = lax.rem(fs, 2), fs // 2
    return chip // RING, lax.rem(chip, RING), core, x


def turn(i, by):
    return lax.rem(i + by + 2 * RING, RING)


def gather_kernel(
    weights, token_slots, tok_ref, gain_in, up_in, down_in, up_ref, down_ref, all_ref,
    gain_ref, up_own, down_own, w_recv, t_recv, w_send, t_send, p_send, p_recv, own_sem,
):
    z, y, core, x = place()
    loads = [
        pltpu.make_async_copy(src, dst, own_sem.at[i])
        for i, (src, dst) in enumerate(
            ((gain_in, gain_ref), (up_in, up_own), (down_in, down_own), (tok_ref, all_ref.at[x]))
        )
    ]
    for load in loads:
        load.start()

    def device(dz=0, dy=0, dx=0, other=False):
        fs = (turn(z, dz) * RING + turn(y, dy)) * 2 + (1 - core if other else core)
        return (fs, turn(x, dx))

    barrier = pltpu.get_barrier_semaphore()
    neighbours = [device(other=True)] + [
        device(**{axis: sign}) for axis in ("dz", "dy", "dx") for sign in (1, -1)
    ]
    for neighbour in neighbours:
        pl.semaphore_signal(barrier, inc=1, device_id=neighbour, device_id_type=MESH)

    rows = up_in.shape[0]
    mine = pl.ds(pl.multiple_of(((z * RING + y) * 2 + core) * rows, rows), rows)
    square = (rows, rows)
    diagonal = lax.broadcasted_iota(jnp.int32, square, 0) == lax.broadcasted_iota(jnp.int32, square, 1)
    for load in loads[:3]:
        load.wait()
    gain = jnp.sum(jnp.where(diagonal, jnp.broadcast_to(gain_ref[...], square), 0.0), axis=1, keepdims=True)
    up_ref[mine, :] = (gain * up_own[...]).astype(BF16)
    down_ref[mine, :] = down_own[...].astype(BF16)
    pl.semaphore_wait(barrier, len(neighbours))

    tables = (up_ref, down_ref)

    def weight_rows(unit):
        matrix, hz, hy, half = unit
        source = (turn(z, -hz) * RING + turn(y, -hy)) * 2 + core
        start = pl.multiple_of(source * rows + half * HALF, HALF)
        return tables[matrix].at[pl.ds(start, HALF), :]

    def weight_copy(index, link, unit):
        ref = weight_rows(unit)
        to = device(**{"d" + link[0]: link[1]})
        return pltpu.make_async_remote_copy(ref, ref, w_send, w_recv.at[index], to, MESH)

    def partner_copy(unit):
        ref = weight_rows(unit)
        return pltpu.make_async_remote_copy(ref, ref, p_send, p_recv.at[unit[0]], device(other=True), MESH)

    def token_copy(index, sign, hops, piece):
        at = pl.ds(piece * PIECE, PIECE)
        there = all_ref.at[turn(x, -sign * hops), at, :]
        here = tok_ref.at[at, :] if hops == 0 else there
        return pltpu.make_async_remote_copy(here, there, t_send, t_recv.at[index], device(dx=sign), MESH)

    w_index = {}
    for leaving in weights:
        for entry in leaving:
            w_index[entry] = len(w_index)
    t_index = {}
    for leaving in token_slots:
        for entry in leaving:
            t_index[entry] = len(t_index)

    def send(slot):
        if slot < len(weights):
            for link, unit in weights[slot]:
                weight_copy(w_index[link, unit], link, unit).start()
        if slot < len(token_slots):
            for entry in token_slots[slot]:
                token_copy(t_index[entry], *entry).start()

    def receive(slot):
        if slot < len(weights):
            for link, unit in weights[slot]:
                matrix, hz, hy, half = unit
                got = (matrix, hz + link[1] * (link[0] == "z"), hy + link[1] * (link[0] == "y"), half)
                ref = weight_rows(got)
                pltpu.make_async_remote_copy(
                    ref, ref, w_send, w_recv.at[w_index[link, unit]], device(other=True), MESH
                ).wait_recv()
                partner_copy(got).start()
        if slot < len(token_slots):
            for sign, hops, piece in token_slots[slot]:
                at = pl.ds(piece * PIECE, PIECE)
                ref = all_ref.at[turn(x, -sign * (hops + 1)), at, :]
                pltpu.make_async_remote_copy(
                    ref, ref, t_send, t_recv.at[t_index[sign, hops, piece]], device(other=True), MESH
                ).wait_recv()

    last = max(len(weights), len(token_slots))
    send(0)
    for matrix in (0, 1):
        for half in (0, 1):
            partner_copy((matrix, 0, 0, half)).start()
    send(1)
    for slot in range(last):
        receive(slot)
        send(slot + 2)

    def settle(ref, sem):
        pltpu.make_async_copy(ref, ref, sem).wait()

    loads[3].wait()
    half_rows = up_ref.shape[0] // 2
    for matrix in (0, 1):
        settle(tables[matrix].at[pl.ds(0, half_rows), :], p_recv.at[matrix])
    for matrix in (0, 1):
        settle(tables[matrix].at[pl.ds(0, half_rows), :], p_send)
        settle(tables[matrix].at[pl.ds(0, len(w_index) // 2 * HALF), :], w_send)
    for _ in range(len(t_index) * PIECE // all_ref.shape[1]):
        settle(all_ref.at[0], t_send)


def apply_kernel(
    up_ref, down_ref, all_ref, out_ref,
    hidden_ref, far_ref, right_ref, left_ref, mine_ref, far_left, far_right, from_left, from_right,
    send_sem, far_recv, near_recv,
):
    z, y, core, x = place()
    fs = (z * RING + y) * 2 + core
    right, left = (fs, turn(x, 1)), (fs, turn(x, -1))
    barrier = pltpu.get_barrier_semaphore()
    for neighbour in (right, left):
        pl.semaphore_signal(barrier, inc=1, device_id=neighbour, device_id_type=MESH)

    sources, tokens, width = all_ref.shape
    features, units = up_ref.shape
    steps, half = tokens // CHUNK, CHUNK // 2
    tile = 512

    def span(step, part=None):
        if part is None:
            return pl.ds(pl.multiple_of(step * CHUNK, CHUNK), CHUNK)
        return pl.ds(pl.multiple_of(step * CHUNK + part * half, half), half)

    def packed(step):
        return pl.ds(pl.multiple_of(step * half, half), half)

    def far_copy(step, part):
        to, dst = (right, far_left) if part == 0 else (left, far_right)
        return pltpu.make_async_remote_copy(
            far_ref.at[span(step, part), :], dst.at[packed(step), :], send_sem, far_recv.at[step, part], to, MESH
        )

    def near_copy(step, side, part):
        to, src, dst = (right, right_ref, from_left) if side == 0 else (left, left_ref, from_right)
        return pltpu.make_async_remote_copy(
            src.at[span(step, part), :], dst.at[span(step, part), :], send_sem, near_recv.at[step, side, part], to, MESH
        )

    def compute(step):
        at = span(step)
        pieces = [all_ref[k, at, :].astype(F32) for k in range(sources)]
        total = sum(jnp.sum(p * p, axis=-1, keepdims=True) for p in pieces)
        scale = lax.rsqrt(total * (1.0 / features) + epsilon)
        normed = [(p * scale).astype(BF16) for p in pieces]
        for t in range(units // tile):
            cols = pl.ds(t * tile, tile)
            acc = jnp.zeros((CHUNK, tile), F32)
            for k in range(sources):
                acc += jnp.dot(normed[k], up_ref[pl.ds(k * width, width), cols], preferred_element_type=F32)
            hidden_ref[:, cols] = jnp.square(jnp.maximum(acc, 0.0)).astype(BF16)

        def block(by):
            cols = pl.ds(pl.multiple_of(turn(x, by) * width, width), width)
            return lax.dot_general(
                hidden_ref[...], down_ref[cols, :], (((1,), (1,)), ((), ())), preferred_element_type=F32
            ).astype(BF16)

        far_ref[at, :] = block(2)
        return block

    def rest(step, block):
        at = span(step)
        right_ref[at, :] = block(1)
        left_ref[at, :] = block(-1)
        mine_ref[at, :] = block(0)

    def pass_on(step):
        for part, buf, got in ((0, right_ref, far_left), (1, left_ref, far_right)):
            far_copy(step, part).wait_recv()
            at = span(step, part)
            buf[at, :] = (buf[at, :].astype(F32) + got[packed(step), :].astype(F32)).astype(BF16)
            near_copy(step, part, part).start()

    def one_step(step, first):
        block = compute(step)
        if first:
            pl.semaphore_wait(barrier, 2)
        for part in (0, 1):
            far_copy(step, part).start()
        rest(step, block)
        near_copy(step, 0, 1).start()
        near_copy(step, 1, 0).start()

    one_step(0, True)

    def body(step, carry):
        one_step(step, False)
        pass_on(step - 1)
        return carry

    lax.fori_loop(1, steps, body, 0)
    pass_on(steps - 1)

    def finish(step, carry):
        for part in (0, 1):
            for side in (0, 1):
                near_copy(step, side, part).wait_recv()
        at = span(step)
        total = mine_ref[at, :].astype(F32) + from_left[at, :].astype(F32) + from_right[at, :].astype(F32)
        out_ref[at, :] = total.astype(BF16)
        return carry

    lax.fori_loop(0, steps, finish, 0)
    for buf in (far_ref, right_ref, left_ref):
        pltpu.make_async_copy(buf, buf, send_sem).wait()


def on_device(tokens, norm_gain, up_weight, down_weight):
    count, width = tokens.shape
    features, units = width * RING, up_weight.shape[1]
    weights, token_slots = weight_plan(), token_plan(count // PIECE)
    vmem = pl.BlockSpec(memory_space=pltpu.VMEM)
    dma = pltpu.SemaphoreType.DMA
    up, down, gathered = pl.pallas_call(
        functools.partial(gather_kernel, weights, token_slots),
        name="gather",
        out_shape=(
            pltpu.VMEM((features, units), BF16),
            pltpu.VMEM((features, units), BF16),
            pltpu.VMEM((RING, count, width), BF16),
        ),
        in_specs=[pl.BlockSpec(memory_space=pltpu.HBM)] * 4,
        out_specs=(vmem, vmem, vmem),
        scratch_shapes=[
            pltpu.VMEM((1, norm_gain.shape[0]), F32), pltpu.VMEM(up_weight.shape, F32), pltpu.VMEM(up_weight.shape, F32),
            dma((sum(map(len, weights)),)), dma((sum(map(len, token_slots)),)), dma, dma, dma, dma((2,)), dma((4,)),
        ],
        compiler_params=pltpu.CompilerParams(collective_id=0, has_side_effects=True, vmem_limit_bytes=36 * 2**20),
    )(tokens, norm_gain[None, :], up_weight, down_weight)
    steps = count // CHUNK
    rows = pltpu.VMEM((count, width), BF16)
    half_rows = pltpu.VMEM((count // 2, width), BF16)
    mixed = pl.pallas_call(
        apply_kernel,
        name="apply",
        out_shape=pltpu.VMEM((count, width), BF16),
        in_specs=[vmem, vmem, vmem],
        out_specs=vmem,
        scratch_shapes=[
            pltpu.VMEM((CHUNK, units), BF16), rows, rows, rows, rows, half_rows, half_rows, rows, rows,
            dma, dma((steps, 2)), dma((steps, 2, 2)),
        ],
        compiler_params=pltpu.CompilerParams(collective_id=1, has_side_effects=True, vmem_limit_bytes=30 * 2**20),
    )(up, down, gathered)
    return up, down, mixed


def solution(mesh):
    return jax.shard_map(
        on_device,
        mesh=mesh,
        in_specs=(P("fs", "tp"), P("fs"), P("fs", "tp"), P("fs", "tp")),
        out_specs=(P(None, "tp"), P(None, "tp"), P("fs", "tp")),
        check_vma=False,
    )
```

```python
import functools

import jax
import jax.numpy as jnp
from jax import lax
from jax.experimental import pallas as pl
from jax.experimental.pallas import tpu as pltpu
from jax.sharding import PartitionSpec as P

epsilon = 1e-06
RING = 4
HALF = 32
PIECE = 128
LAG = 3
CHUNK = 256
MESH = pl.DeviceIdType.MESH
F32, BF16 = jnp.float32, jnp.bfloat16


def onward(at, first, second, half):
    links = []
    if at[second] == 0:
        if at[first] == 0:
            links += [(first, 1), (first, -1)]
        elif at[first] == 1 and half == 0:
            links += [(first, 1)]
        elif at[first] == -1 and half == 1:
            links += [(first, -1)]
        links += [(second, 1), (second, -1)]
    elif at[second] == 1 and half == 0:
        links += [(second, 1)]
    elif at[second] == -1 and half == 1:
        links += [(second, -1)]
    return links


def weight_plan():
    links = [(axis, sign) for axis in "yz" for sign in (1, -1)]
    queues = {link: [] for link in links}

    def offer(unit, slot):
        matrix, z, y, half = unit
        first, second = ("y", "z") if matrix == 0 else ("z", "y")
        for link in onward({"z": z, "y": y}, first, second, half):
            queues[link].append((0 if link[0] == first else 1, slot, unit))

    for half in (0, 1):
        for matrix in (0, 1):
            offer((matrix, 0, 0, half), 0)
    slots, landed = [], {}
    while any(queues.values()) or any(landed.values()):
        now = len(slots)
        for unit in landed.pop(now - LAG, []):
            offer(unit, now)
        leaving = []
        for link in links:
            if queues[link]:
                choice = min(queues[link], key=lambda entry: entry[:2])
                queues[link].remove(choice)
                leaving.append((link, choice[2]))
        landed[now] = []
        for (axis, sign), (matrix, z, y, half) in leaving:
            landed[now].append((matrix, z + sign * (axis == "z"), y + sign * (axis == "y"), half))
        slots.append(leaving)
        if len(slots) > 100:
            raise ValueError("plan")
    while slots and not slots[-1]:
        slots.pop()
    return slots


def token_plan(pieces):
    own = {1: list(range(pieces)), -1: list(range(pieces))}
    passing = {1: [], -1: []}
    slots, landed = [], {}
    while own[1] or own[-1] or passing[1] or passing[-1] or any(landed.values()):
        now = len(slots)
        for sign, hops, piece in landed.pop(now - LAG, []):
            if hops == 1 and (piece % 2 == 0) == (sign == 1):
                passing[sign].append(piece)
        leaving = []
        for sign in (1, -1):
            if passing[sign]:
                leaving.append((sign, 1, passing[sign].pop(0)))
            elif own[sign]:
                leaving.append((sign, 0, own[sign].pop(0)))
        landed[now] = [(sign, hops + 1, piece) for sign, hops, piece in leaving]
        slots.append(leaving)
    while slots and not slots[-1]:
        slots.pop()
    return slots


def place():
    fs, x = lax.axis_index("fs"), lax.axis_index("tp")
    core, chip = lax.rem(fs, 2), fs // 2
    return chip // RING, lax.rem(chip, RING), core, x


def turn(i, by):
    return lax.rem(i + by + 2 * RING, RING)


def layer_kernel(
    weights, token_slots, tok_ref, gain_in, up_in, down_in, up_ref, down_ref, out_ref,
    gain_ref, up_own, down_own, all_ref,
    hidden_ref, far_ref, right_ref, left_ref, mine_ref, far_left, far_right, from_left, from_right,
    w_recv, t_recv, w_send, t_send, p_send, p_recv, own_sem, send_sem, far_recv, near_recv,
):
    z, y, core, x = place()
    loads = [
        pltpu.make_async_copy(src, dst, own_sem.at[i])
        for i, (src, dst) in enumerate(
            ((gain_in, gain_ref), (up_in, up_own), (down_in, down_own), (tok_ref, all_ref.at[x]))
        )
    ]
    for load in loads:
        load.start()

    def device(dz=0, dy=0, dx=0, other=False):
        fs = (turn(z, dz) * RING + turn(y, dy)) * 2 + (1 - core if other else core)
        return (fs, turn(x, dx))

    barrier = pltpu.get_barrier_semaphore()
    neighbours = [device(other=True)] + [
        device(**{axis: sign}) for axis in ("dz", "dy", "dx") for sign in (1, -1)
    ]
    for neighbour in neighbours:
        pl.semaphore_signal(barrier, inc=1, device_id=neighbour, device_id_type=MESH)

    rows = up_in.shape[0]
    tables = (up_ref, down_ref)

    def weight_rows(unit):
        matrix, hz, hy, half = unit
        source = (turn(z, -hz) * RING + turn(y, -hy)) * 2 + core
        start = pl.multiple_of(source * rows + half * HALF, HALF)
        return tables[matrix].at[pl.ds(start, HALF), :]

    def weight_copy(index, link, unit):
        ref = weight_rows(unit)
        to = device(**{"d" + link[0]: link[1]})
        return pltpu.make_async_remote_copy(ref, ref, w_send, w_recv.at[index], to, MESH)

    def partner_copy(unit):
        ref = weight_rows(unit)
        return pltpu.make_async_remote_copy(ref, ref, p_send, p_recv.at[unit[0]], device(other=True), MESH)

    def token_copy(index, sign, hops, piece):
        at = pl.ds(piece * PIECE, PIECE)
        there = all_ref.at[turn(x, -sign * hops), at, :]
        here = tok_ref.at[at, :] if hops == 0 else there
        return pltpu.make_async_remote_copy(here, there, t_send, t_recv.at[index], device(dx=sign), MESH)

    w_index = {}
    for leaving in weights:
        for entry in leaving:
            w_index[entry] = len(w_index)
    t_index = {}
    for leaving in token_slots:
        for entry in leaving:
            t_index[entry] = len(t_index)

    def send_weights(slot):
        if slot < len(weights):
            for link, unit in weights[slot]:
                weight_copy(w_index[link, unit], link, unit).start()

    def send_tokens(slot):
        if slot < len(token_slots):
            for entry in token_slots[slot]:
                token_copy(t_index[entry], *entry).start()

    def receive_weights(slot):
        if slot < len(weights):
            for link, unit in weights[slot]:
                matrix, hz, hy, half = unit
                got = (matrix, hz + link[1] * (link[0] == "z"), hy + link[1] * (link[0] == "y"), half)
                ref = weight_rows(got)
                pltpu.make_async_remote_copy(
                    ref, ref, w_send, w_recv.at[w_index[link, unit]], device(other=True), MESH
                ).wait_recv()
                partner_copy(got).start()

    def receive_tokens(slot):
        for sign, hops, piece in token_slots[slot]:
            at = pl.ds(piece * PIECE, PIECE)
            ref = all_ref.at[turn(x, -sign * (hops + 1)), at, :]
            pltpu.make_async_remote_copy(
                ref, ref, t_send, t_recv.at[t_index[sign, hops, piece]], device(other=True), MESH
            ).wait_recv()

    pl.semaphore_wait(barrier, len(neighbours))
    for slot in range(LAG):
        send_tokens(slot)
    mine = pl.ds(pl.multiple_of(((z * RING + y) * 2 + core) * rows, rows), rows)
    square = (rows, rows)
    diagonal = lax.broadcasted_iota(jnp.int32, square, 0) == lax.broadcasted_iota(jnp.int32, square, 1)
    for load in loads[:3]:
        load.wait()
    gain = jnp.sum(jnp.where(diagonal, jnp.broadcast_to(gain_ref[...], square), 0.0), axis=1, keepdims=True)
    up_ref[mine, :] = (gain * up_own[...]).astype(BF16)
    down_ref[mine, :] = down_own[...].astype(BF16)
    for slot in range(LAG):
        send_weights(slot)
    for matrix in (0, 1):
        for half in (0, 1):
            partner_copy((matrix, 0, 0, half)).start()
    early = len(weights)
    for slot in range(early):
        receive_weights(slot)
        receive_tokens(slot)
        send_weights(slot + LAG)
        send_tokens(slot + LAG)

    def settle(ref, sem):
        pltpu.make_async_copy(ref, ref, sem).wait()

    loads[3].wait()
    half_rows = up_ref.shape[0] // 2
    for matrix in (0, 1):
        settle(tables[matrix].at[pl.ds(0, half_rows), :], p_recv.at[matrix])

    right, left = device(dx=1), device(dx=-1)
    sources, tokens, width = all_ref.shape
    features, units = up_ref.shape
    steps, half = tokens // CHUNK, CHUNK // 2
    tile = 512

    def span(step, part=None):
        if part is None:
            return pl.ds(pl.multiple_of(step * CHUNK, CHUNK), CHUNK)
        return pl.ds(pl.multiple_of(step * CHUNK + part * half, half), half)

    def packed(step):
        return pl.ds(pl.multiple_of(step * half, half), half)

    def far_copy(step, part):
        to, dst = (right, far_left) if part == 0 else (left, far_right)
        return pltpu.make_async_remote_copy(
            far_ref.at[span(step, part), :], dst.at[packed(step), :], send_sem, far_recv.at[step, part], to, MESH
        )

    def near_copy(step, side, part):
        to, src, dst = (right, right_ref, from_left) if side == 0 else (left, left_ref, from_right)
        return pltpu.make_async_remote_copy(
            src.at[span(step, part), :], dst.at[span(step, part), :], send_sem, near_recv.at[step, side, part], to, MESH
        )

    def compute(step):
        at = span(step)
        pieces = [all_ref[k, at, :].astype(F32) for k in range(sources)]
        total = sum(jnp.sum(p * p, axis=-1, keepdims=True) for p in pieces)
        scale = lax.rsqrt(total * (1.0 / features) + epsilon)
        normed = [(p * scale).astype(BF16) for p in pieces]
        for t in range(units // tile):
            cols = pl.ds(t * tile, tile)
            acc = jnp.zeros((CHUNK, tile), F32)
            for k in range(sources):
                acc += jnp.dot(normed[k], up_ref[pl.ds(k * width, width), cols], preferred_element_type=F32)
            hidden_ref[:, cols] = jnp.square(jnp.maximum(acc, 0.0)).astype(BF16)

        def block(by):
            cols = pl.ds(pl.multiple_of(turn(x, by) * width, width), width)
            return lax.dot_general(
                hidden_ref[...], down_ref[cols, :], (((1,), (1,)), ((), ())), preferred_element_type=F32
            ).astype(BF16)

        far_ref[at, :] = block(2)
        return block

    def rest(step, block):
        at = span(step)
        right_ref[at, :] = block(1)
        left_ref[at, :] = block(-1)
        mine_ref[at, :] = block(0)

    def pass_on(step):
        for part, buf, got in ((0, right_ref, far_left), (1, left_ref, far_right)):
            far_copy(step, part).wait_recv()
            at = span(step, part)
            buf[at, :] = (buf[at, :].astype(F32) + got[packed(step), :].astype(F32)).astype(BF16)
            near_copy(step, part, part).start()

    def one_step(step):
        block = compute(step)
        for part in (0, 1):
            far_copy(step, part).start()
        return block

    def two_step(step, block):
        rest(step, block)
        near_copy(step, 0, 1).start()
        near_copy(step, 1, 0).start()

    block = one_step(0)
    for slot in range(early, len(token_slots) - LAG):
        receive_tokens(slot)
        send_tokens(slot + LAG)
    two_step(0, block)
    late = range(max(early, len(token_slots) - LAG), len(token_slots))
    needed = min(piece for slot in late for _, _, piece in token_slots[slot]) * PIECE // CHUNK

    def body(step, carry):
        @pl.when(step == needed)
        def _():
            for slot in late:
                receive_tokens(slot)

        two_step(step, one_step(step))
        pass_on(step - 1)
        return carry

    lax.fori_loop(1, steps, body, 0)
    pass_on(steps - 1)

    def finish(step, carry):
        for part in (0, 1):
            for side in (0, 1):
                near_copy(step, side, part).wait_recv()
        at = span(step)
        total = mine_ref[at, :].astype(F32) + from_left[at, :].astype(F32) + from_right[at, :].astype(F32)
        out_ref[at, :] = total.astype(BF16)
        return carry

    lax.fori_loop(0, steps, finish, 0)
    for buf in (far_ref, right_ref, left_ref):
        pltpu.make_async_copy(buf, buf, send_sem).wait()
    for matrix in (0, 1):
        settle(tables[matrix].at[pl.ds(0, half_rows), :], p_send)
        settle(tables[matrix].at[pl.ds(0, len(w_index) // 2 * HALF), :], w_send)
    for _ in range(len(t_index) * PIECE // all_ref.shape[1]):
        settle(all_ref.at[0], t_send)


def store_kernel(up_ref, down_ref, mixed_ref, up_out, down_out, mixed_out, sem):
    copies = [
        pltpu.make_async_copy(src, dst, sem.at[i])
        for i, (src, dst) in enumerate(((up_ref, up_out), (down_ref, down_out), (mixed_ref, mixed_out)))
    ]
    for copy in copies:
        copy.start()
    for copy in copies:
        copy.wait()


def on_device(tokens, norm_gain, up_weight, down_weight):
    count, width = tokens.shape
    features, units = width * RING, up_weight.shape[1]
    weights, token_slots = weight_plan(), token_plan(count // PIECE)
    steps = count // CHUNK
    vmem, hbm = pl.BlockSpec(memory_space=pltpu.VMEM), pl.BlockSpec(memory_space=pltpu.HBM)
    dma = pltpu.SemaphoreType.DMA
    rows, half_rows = pltpu.VMEM((count, width), BF16), pltpu.VMEM((count // 2, width), BF16)
    shapes = ((features, units), (features, units), (count, width))
    results = pl.pallas_call(
        functools.partial(layer_kernel, weights, token_slots),
        name="layer",
        out_shape=[pltpu.VMEM(shape, BF16) for shape in shapes],
        in_specs=[hbm] * 4,
        out_specs=[vmem] * 3,
        scratch_shapes=[
            pltpu.VMEM((1, norm_gain.shape[0]), F32), pltpu.VMEM(up_weight.shape, F32), pltpu.VMEM(up_weight.shape, F32),
            pltpu.VMEM((RING, count, width), BF16),
            pltpu.VMEM((CHUNK, units), BF16), rows, rows, rows, rows, half_rows, half_rows, rows, rows,
            dma((sum(map(len, weights)),)), dma((sum(map(len, token_slots)),)), dma, dma, dma, dma((2,)), dma((4,)),
            dma, dma((steps, 2)), dma((steps, 2, 2)),
        ],
        compiler_params=pltpu.CompilerParams(collective_id=0, has_side_effects=True, vmem_limit_bytes=42 * 2**20),
    )(tokens, norm_gain[None, :], up_weight, down_weight)
    return pl.pallas_call(
        store_kernel,
        name="store",
        out_shape=[jax.ShapeDtypeStruct(shape, BF16) for shape in shapes],
        in_specs=[vmem] * 3,
        out_specs=[hbm] * 3,
        scratch_shapes=[dma((3,))],
        compiler_params=pltpu.CompilerParams(vmem_limit_bytes=2**20),
    )(*results)


def solution(mesh):
    return jax.shard_map(
        on_device,
        mesh=mesh,
        in_specs=(P("fs", "tp"), P("fs"), P("fs", "tp"), P("fs", "tp")),
        out_specs=(P(None, "tp"), P(None, "tp"), P("fs", "tp")),
        check_vma=False,
    )
```

```python
import functools

import jax
import jax.numpy as jnp
from jax import lax
from jax.experimental import pallas as pl
from jax.experimental.pallas import tpu as pltpu
from jax.sharding import PartitionSpec as P

epsilon = 1e-06
RING = 4
HALF = 32
PIECE = 128
LAG = 3
TOKEN_LAG = 6
TURN = 2
PACE = {0: (2,) * 3 + (1,) * 12, 1: (0,) * 3 + (1,) * 12}
CHUNK = 256
MESH = pl.DeviceIdType.MESH
F32, BF16 = jnp.float32, jnp.bfloat16


def onward(at, first, second, half):
    links = []
    if at[second] == 0:
        if at[first] == 0:
            links += [(first, 1), (first, -1)]
        elif at[first] == 1 and half == 0:
            links += [(first, 1)]
        elif at[first] == -1 and half == 1:
            links += [(first, -1)]
        links += [(second, 1), (second, -1)]
    elif at[second] == 1 and half == 0:
        links += [(second, 1)]
    elif at[second] == -1 and half == 1:
        links += [(second, -1)]
    return links


def weight_plan():
    links = [(axis, sign) for axis in "yz" for sign in (1, -1)]
    queues = {link: [] for link in links}

    def offer(unit, slot):
        matrix, z, y, half = unit
        first, second = ("y", "z") if matrix == 0 else ("z", "y")
        for link in onward({"z": z, "y": y}, first, second, half):
            queues[link].append((0 if link[0] == first else 1, slot, unit))

    for half in (0, 1):
        for matrix in (0, 1):
            offer((matrix, 0, 0, half), 0)
    slots, landed = [], {}
    while any(queues.values()) or any(landed.values()):
        now = len(slots)
        for unit in landed.pop(now - LAG, []):
            offer(unit, now)
        leaving = []
        for link in links:
            if queues[link]:
                choice = min(queues[link], key=lambda entry: entry[:2])
                queues[link].remove(choice)
                leaving.append((link, choice[2]))
        landed[now] = []
        for (axis, sign), (matrix, z, y, half) in leaving:
            landed[now].append((matrix, z + sign * (axis == "z"), y + sign * (axis == "y"), half))
        slots.append(leaving)
        if len(slots) > 100:
            raise ValueError("plan")
    while slots and not slots[-1]:
        slots.pop()
    return slots


def token_plan(pieces):
    evens, odds = list(range(0, pieces, 2)), list(range(1, pieces, 2))
    own = {1: evens + odds, -1: odds + evens}
    passing = {1: [], -1: []}
    slots, landed = [], {}
    while own[1] or own[-1] or passing[1] or passing[-1] or any(landed.values()):
        now = len(slots)
        for sign, hops, piece in landed.pop(now - TOKEN_LAG, []):
            if hops == 1 and (piece % 2 == 0) == (sign == 1):
                passing[sign].append(piece)
        leaving = []
        for sign in (1, -1):
            if passing[sign]:
                leaving.append((sign, 1, passing[sign].pop(0)))
            elif own[sign]:
                leaving.append((sign, 0, own[sign].pop(0)))
        landed[now] = [(sign, hops + 1, piece) for sign, hops, piece in leaving]
        slots.append(leaving)
    while slots and not slots[-1]:
        slots.pop()
    return slots


def place():
    fs, x = lax.axis_index("fs"), lax.axis_index("tp")
    core, chip = lax.rem(fs, 2), fs // 2
    return chip // RING, lax.rem(chip, RING), core, x


def turn(i, by):
    return lax.rem(i + by + 2 * RING, RING)


def gather_kernel(
    weights, token_slots, tok_ref, gain_in, up_in, down_in, up_ref, down_ref, all_ref,
    gain_ref, up_own, down_own, w_recv, t_recv, w_send, t_send, p_send, p_recv, own_sem,
):
    z, y, core, x = place()
    loads = [
        pltpu.make_async_copy(src, dst, own_sem.at[i])
        for i, (src, dst) in enumerate(
            ((gain_in, gain_ref), (up_in, up_own), (down_in, down_own), (tok_ref, all_ref.at[x]))
        )
    ]
    for load in loads:
        load.start()

    def device(dz=0, dy=0, dx=0, other=False):
        fs = (turn(z, dz) * RING + turn(y, dy)) * 2 + (1 - core if other else core)
        return (fs, turn(x, dx))

    barrier = pltpu.get_barrier_semaphore()
    neighbours = [device(other=True)] + [
        device(**{axis: sign}) for axis in ("dz", "dy", "dx") for sign in (1, -1)
    ]
    for neighbour in neighbours:
        pl.semaphore_signal(barrier, inc=1, device_id=neighbour, device_id_type=MESH)

    rows = up_in.shape[0]
    tables = (up_ref, down_ref)

    def weight_rows(unit):
        matrix, hz, hy, half = unit
        source = (turn(z, -hz) * RING + turn(y, -hy)) * 2 + core
        start = pl.multiple_of(source * rows + half * HALF, HALF)
        return tables[matrix].at[pl.ds(start, HALF), :]

    def weight_copy(index, link, unit):
        ref = weight_rows(unit)
        to = device(**{"d" + link[0]: link[1]})
        return pltpu.make_async_remote_copy(ref, ref, w_send, w_recv.at[index], to, MESH)

    def partner_copy(unit):
        ref = weight_rows(unit)
        return pltpu.make_async_remote_copy(ref, ref, p_send, p_recv.at[unit[0]], device(other=True), MESH)

    def token_copy(index, sign, hops, piece):
        at = pl.ds(piece * PIECE, PIECE)
        there = all_ref.at[turn(x, -sign * hops), at, :]
        here = tok_ref.at[at, :] if hops == 0 else there
        return pltpu.make_async_remote_copy(here, there, t_send, t_recv.at[index], device(dx=sign), MESH)

    w_index = {}
    for leaving in weights:
        for entry in leaving:
            w_index[entry] = len(w_index)
    t_index = {}
    for leaving in token_slots:
        for entry in leaving:
            t_index[entry] = len(t_index)

    def send_weights(slot):
        if slot < len(weights):
            for link, unit in weights[slot]:
                weight_copy(w_index[link, unit], link, unit).start()

    def send_tokens(slot):
        if slot < len(token_slots):
            for entry in token_slots[slot]:
                token_copy(t_index[entry], *entry).start()

    def receive_weights(slot):
        for link, unit in weights[slot]:
            matrix, hz, hy, half = unit
            got = (matrix, hz + link[1] * (link[0] == "z"), hy + link[1] * (link[0] == "y"), half)
            ref = weight_rows(got)
            pltpu.make_async_remote_copy(
                ref, ref, w_send, w_recv.at[w_index[link, unit]], device(other=True), MESH
            ).wait_recv()
            partner_copy(got).start()

    def receive_tokens(slot):
        for sign, hops, piece in token_slots[slot]:
            at = pl.ds(piece * PIECE, PIECE)
            ref = all_ref.at[turn(x, -sign * (hops + 1)), at, :]
            pltpu.make_async_remote_copy(
                ref, ref, t_send, t_recv.at[t_index[sign, hops, piece]], device(other=True), MESH
            ).wait_recv()

    def first_tokens():
        for slot in range(TOKEN_LAG):
            send_tokens(slot)

    def next_tokens(slot):
        if slot < len(token_slots):
            receive_tokens(slot)
            send_tokens(slot + TOKEN_LAG)

    pl.semaphore_wait(barrier, len(neighbours))

    @pl.when(core == 0)
    def _():
        first_tokens()

    mine = pl.ds(pl.multiple_of(((z * RING + y) * 2 + core) * rows, rows), rows)
    square = (rows, rows)
    diagonal = lax.broadcasted_iota(jnp.int32, square, 0) == lax.broadcasted_iota(jnp.int32, square, 1)
    for load in loads[:3]:
        load.wait()
    gain = jnp.sum(jnp.where(diagonal, jnp.broadcast_to(gain_ref[...], square), 0.0), axis=1, keepdims=True)
    up_ref[mine, :] = (gain * up_own[...]).astype(BF16)
    down_ref[mine, :] = down_own[...].astype(BF16)
    for slot in range(LAG):
        send_weights(slot)
    for matrix in (0, 1):
        for half in (0, 1):
            partner_copy((matrix, 0, 0, half)).start()
    done = {0: 0, 1: 0}
    for slot in range(len(weights)):
        receive_weights(slot)
        send_weights(slot + LAG)
        for which in (0, 1):
            steps = range(done[which], min(done[which] + PACE[which][slot], len(token_slots)))
            done[which] = max(done[which], steps.stop)
            if steps or (which == 1 and slot == TURN):

                @pl.when(core == which)
                def _(slot=slot, which=which, steps=steps):
                    if which == 1 and slot == TURN:
                        first_tokens()
                    for step in steps:
                        next_tokens(step)

    for which in (0, 1):

        @pl.when(core == which)
        def _(which=which):
            for step in range(done[which], len(token_slots)):
                next_tokens(step)

    def settle(ref, sem):
        pltpu.make_async_copy(ref, ref, sem).wait()

    loads[3].wait()
    half_rows = up_ref.shape[0] // 2
    for matrix in (0, 1):
        settle(tables[matrix].at[pl.ds(0, half_rows), :], p_recv.at[matrix])
    for matrix in (0, 1):
        settle(tables[matrix].at[pl.ds(0, half_rows), :], p_send)
        settle(tables[matrix].at[pl.ds(0, len(w_index) // 2 * HALF), :], w_send)
    for _ in range(len(t_index) * PIECE // all_ref.shape[1]):
        settle(all_ref.at[0], t_send)


def products(x, all_ref, up_ref, down_ref, hidden_ref, at):
    sources, _, width = all_ref.shape
    features, units = up_ref.shape
    tile = 512
    pieces = [all_ref[k, at, :].astype(F32) for k in range(sources)]
    total = sum(jnp.sum(p * p, axis=-1, keepdims=True) for p in pieces)
    scale = lax.rsqrt(total * (1.0 / features) + epsilon)
    normed = [(p * scale).astype(BF16) for p in pieces]
    for t in range(units // tile):
        cols = pl.ds(t * tile, tile)
        acc = jnp.zeros((CHUNK, tile), F32)
        for k in range(sources):
            acc += jnp.dot(normed[k], up_ref[pl.ds(k * width, width), cols], preferred_element_type=F32)
        hidden_ref[:, cols] = jnp.square(jnp.maximum(acc, 0.0)).astype(BF16)

    def block(by):
        cols = pl.ds(pl.multiple_of(turn(x, by) * width, width), width)
        return lax.dot_general(
            hidden_ref[...], down_ref[cols, :], (((1,), (1,)), ((), ())), preferred_element_type=F32
        ).astype(BF16)

    return block


TARGETS = (2, 1, -1, 0)


def store_kernel(which, up_ref, down_ref, *refs):
    *extra, up_out, down_out = refs[:-1] if len(refs) == 3 else (refs[0], *refs[3:5])
    sem = refs[-1]
    copies = []
    for m, (src, dst) in enumerate(((up_ref, up_out), (down_ref, down_out))):
        part = src.shape[0] // 4
        for i in range(4):
            at = pl.ds(i * part, part)
            copies.append(pltpu.make_async_copy(src.at[at, :], dst.at[at, :], sem.at[m * 4 + i]))

    if extra:
        more = pltpu.make_async_copy(extra[0], refs[5], sem.at[8])
        more.start()

    @pl.when(lax.rem(lax.axis_index("fs"), 2) == which)
    def _():
        for copy in copies:
            copy.start()
        for copy in copies:
            copy.wait()

    if extra:
        more.wait()


def apply_kernel(
    up_ref, down_ref, all_ref, stored_ref, out_ref,
    hidden_ref, far_ref, right_ref, left_ref, mine_ref, far_left, far_right, from_left, from_right,
    send_sem, far_recv, near_recv,
):
    z, y, core, x = place()
    fs = (z * RING + y) * 2 + core
    right, left = (fs, turn(x, 1)), (fs, turn(x, -1))
    barrier = pltpu.get_barrier_semaphore()
    for neighbour in (right, left):
        pl.semaphore_signal(barrier, inc=1, device_id=neighbour, device_id_type=MESH)

    tokens, width = out_ref.shape
    steps, half = tokens // CHUNK, CHUNK // 2

    def span(step, part=None):
        if part is None:
            return pl.ds(pl.multiple_of(step * CHUNK, CHUNK), CHUNK)
        return pl.ds(pl.multiple_of(step * CHUNK + part * half, half), half)

    def packed(step):
        return pl.ds(pl.multiple_of(step * half, half), half)

    def far_copy(step, part):
        to, dst = (right, far_left) if part == 0 else (left, far_right)
        return pltpu.make_async_remote_copy(
            far_ref.at[span(step, part), :], dst.at[packed(step), :], send_sem, far_recv.at[step, part], to, MESH
        )

    def near_copy(step, side, part):
        to, src, dst = (right, right_ref, from_left) if side == 0 else (left, left_ref, from_right)
        return pltpu.make_async_remote_copy(
            src.at[span(step, part), :], dst.at[span(step, part), :], send_sem, near_recv.at[step, side, part], to, MESH
        )

    def pass_on(step):
        for part, buf, got in ((0, right_ref, far_left), (1, left_ref, far_right)):
            far_copy(step, part).wait_recv()
            at = span(step, part)
            buf[at, :] = (buf[at, :].astype(F32) + got[packed(step), :].astype(F32)).astype(BF16)
            near_copy(step, part, part).start()

    partials = (far_ref, right_ref, left_ref, mine_ref)

    def send_far(step):
        for part in (0, 1):
            far_copy(step, part).start()

    def send_near(step):
        near_copy(step, 0, 1).start()
        near_copy(step, 1, 0).start()

    def multiply(step, first):
        at = span(step)
        block = products(x, all_ref, up_ref, down_ref, hidden_ref, at)
        far_ref[at, :] = block(TARGETS[0])
        if first:
            pl.semaphore_wait(barrier, 2)
        send_far(step)
        if not first:
            pass_on(step - 1)
        for buf, by in zip(partials[1:], TARGETS[1:]):
            buf[at, :] = block(by)
        send_near(step)

    multiply(0, True)

    def body(step, carry):
        multiply(step, False)
        return carry

    lax.fori_loop(1, steps, body, 0)
    pass_on(steps - 1)

    def finish(step, carry):
        for part in (0, 1):
            for side in (0, 1):
                near_copy(step, side, part).wait_recv()
        at = span(step)
        total = mine_ref[at, :].astype(F32) + from_left[at, :].astype(F32) + from_right[at, :].astype(F32)
        out_ref[at, :] = total.astype(BF16)
        return carry

    lax.fori_loop(0, steps, finish, 0)
    for buf in (far_ref, right_ref, left_ref):
        pltpu.make_async_copy(buf, buf, send_sem).wait()


def on_device(tokens, norm_gain, up_weight, down_weight):
    count, width = tokens.shape
    features, units = width * RING, up_weight.shape[1]
    weights, token_slots = weight_plan(), token_plan(count // PIECE)
    steps = count // CHUNK
    vmem, hbm = pl.BlockSpec(memory_space=pltpu.VMEM), pl.BlockSpec(memory_space=pltpu.HBM)
    dma = pltpu.SemaphoreType.DMA
    matrix = (features, units)
    hidden = pltpu.VMEM((CHUNK, units), BF16)
    up, down, gathered = pl.pallas_call(
        functools.partial(gather_kernel, weights, token_slots),
        name="gather",
        out_shape=[pltpu.VMEM(matrix, BF16), pltpu.VMEM(matrix, BF16), pltpu.VMEM((RING, count, width), BF16)],
        in_specs=[hbm] * 4,
        out_specs=[vmem] * 3,
        scratch_shapes=[
            pltpu.VMEM((1, norm_gain.shape[0]), F32), pltpu.VMEM(up_weight.shape, F32), pltpu.VMEM(up_weight.shape, F32),
            dma((sum(map(len, weights)),)), dma((sum(map(len, token_slots)),)), dma, dma, dma, dma((2,)), dma((4,)),
        ],
        compiler_params=pltpu.CompilerParams(collective_id=0, has_side_effects=True, vmem_limit_bytes=33 * 2**20),
    )(tokens, norm_gain[None, :], up_weight, down_weight)
    whole = jax.ShapeDtypeStruct(matrix, BF16)

    def pinned(*arrays):
        return [pltpu.with_memory_space_constraint(a, pltpu.VMEM) for a in arrays]

    stored = pl.pallas_call(
        functools.partial(store_kernel, 1),
        name="store",
        out_shape=[whole, whole],
        in_specs=[vmem] * 2,
        out_specs=[hbm] * 2,
        scratch_shapes=[dma((8,))],
        compiler_params=pltpu.CompilerParams(vmem_limit_bytes=8 * 2**20),
    )(*pinned(up, down))
    rows, half_rows = pltpu.VMEM((count, width), BF16), pltpu.VMEM((count // 2, width), BF16)
    mixed = pl.pallas_call(
        apply_kernel,
        name="apply",
        out_shape=pltpu.VMEM((count, width), BF16),
        in_specs=[vmem] * 3 + [hbm],
        out_specs=vmem,
        scratch_shapes=[
            hidden, rows, rows, rows, rows, half_rows, half_rows, rows, rows,
            dma, dma((steps, 2)), dma((steps, 2, 2)),
        ],
        compiler_params=pltpu.CompilerParams(collective_id=1, has_side_effects=True, vmem_limit_bytes=31 * 2**20),
    )(*pinned(up, down, gathered), stored[0])
    return pl.pallas_call(
        functools.partial(store_kernel, 0),
        name="finish",
        out_shape=[whole, whole, jax.ShapeDtypeStruct((count, width), BF16)],
        in_specs=[vmem] * 3 + [hbm] * 2,
        out_specs=[hbm] * 3,
        scratch_shapes=[dma((9,))],
        input_output_aliases={3: 0, 4: 1},
        compiler_params=pltpu.CompilerParams(vmem_limit_bytes=8 * 2**20),
    )(*pinned(up, down, mixed), *stored)


def solution(mesh):
    return jax.shard_map(
        on_device,
        mesh=mesh,
        in_specs=(P("fs", "tp"), P("fs"), P("fs", "tp"), P("fs", "tp")),
        out_specs=(P(None, "tp"), P(None, "tp"), P("fs", "tp")),
        check_vma=False,
    )
```

```python
import functools

import jax
import jax.numpy as jnp
from jax import lax
from jax.experimental import pallas as pl
from jax.experimental.pallas import tpu as pltpu
from jax.sharding import PartitionSpec as P

epsilon = 1e-06
RING = 4
UNIT = 16
PIECE = 128
LAG = 5
TOKEN_LAG = 6
TURN = 6
PACE = ((1,) * 6 + (1, 0) * 13, (0,) * 7 + (1, 0) * 12 + (0,))
READY = 18
HIDE = ({18 + 2 * i: i for i in range(6)}, {22: 0, 26: 1, 30: 2})
CHUNK = 256
MESH = pl.DeviceIdType.MESH
F32, BF16 = jnp.float32, jnp.bfloat16


def onward(at, first, second, half):
    links = []
    if at[second] == 0:
        if at[first] == 0:
            links += [(first, 1), (first, -1)]
        elif at[first] == 1 and half == 0:
            links += [(first, 1)]
        elif at[first] == -1 and half == 1:
            links += [(first, -1)]
        links += [(second, 1), (second, -1)]
    elif at[second] == 1 and half == 0:
        links += [(second, 1)]
    elif at[second] == -1 and half == 1:
        links += [(second, -1)]
    return links


def weight_plan():
    links = [(axis, sign) for axis in "yz" for sign in (1, -1)]
    queues = {link: [] for link in links}

    def offer(unit, slot):
        matrix, order, z, y, half = unit
        first, second = ("y", "z") if order == 0 else ("z", "y")
        for link in onward({"z": z, "y": y}, first, second, half):
            queues[link].append((matrix, 0 if link[0] == first else 1, slot, unit))

    for half in (0, 1):
        for matrix in (0, 1):
            for order in (0, 1):
                offer((matrix, order, 0, 0, half), 0)
    slots, landed = [], {}
    while any(queues.values()) or any(landed.values()):
        now = len(slots)
        for unit in landed.pop(now - LAG, []):
            offer(unit, now)
        leaving = []
        for link in links:
            if queues[link]:
                choice = min(queues[link], key=lambda entry: entry[:3])
                queues[link].remove(choice)
                leaving.append((link, choice[3]))
        landed[now] = [arrived(link, unit) for link, unit in leaving]
        slots.append(leaving)
    while slots and not slots[-1]:
        slots.pop()
    return slots


def arrived(link, unit):
    (axis, sign), (matrix, order, z, y, half) = link, unit
    return (matrix, order, z + sign * (axis == "z"), y + sign * (axis == "y"), half)


def token_plan(pieces, sorted_first):
    own = {sign: list(range(pieces)) for sign in (1, -1)}
    if sorted_first:
        for sign in own:
            own[sign].sort(key=lambda piece: (piece % 2 == 0) != (sign == 1))
    passing = {1: [], -1: []}
    slots, landed = [], {}
    while own[1] or own[-1] or passing[1] or passing[-1] or any(landed.values()):
        now = len(slots)
        for sign, hops, piece in landed.pop(now - TOKEN_LAG, []):
            if hops == 1 and (piece % 2 == 0) == (sign == 1):
                passing[sign].append(piece)
        leaving = []
        for sign in (1, -1):
            if passing[sign]:
                leaving.append((sign, 1, passing[sign].pop(0)))
            elif own[sign]:
                leaving.append((sign, 0, own[sign].pop(0)))
        landed[now] = [(sign, hops + 1, piece) for sign, hops, piece in leaving]
        slots.append(leaving)
    while slots and not slots[-1]:
        slots.pop()
    return slots


def place():
    fs, x = lax.axis_index("fs"), lax.axis_index("tp")
    core, chip = lax.rem(fs, 2), fs // 2
    return chip // RING, lax.rem(chip, RING), core, x


def turn(i, by):
    return lax.rem(i + by + 2 * RING, RING)


def gather_kernel(
    weights, token_slots, tok_ref, gain_in, up_in, down_in, up_ref, down_ref, hidden_ref,
    all_ref, gain_ref, up_own, down_own, w_recv, t_recv, w_send, t_send, p_send, p_recv, own_sem,
):
    z, y, core, x = place()
    loads = [
        pltpu.make_async_copy(src, dst, own_sem.at[i])
        for i, (src, dst) in enumerate(
            ((gain_in, gain_ref), (up_in, up_own), (down_in, down_own), (tok_ref, all_ref.at[x]))
        )
    ]
    for load in loads:
        load.start()

    def device(dz=0, dy=0, dx=0, other=False):
        fs = (turn(z, dz) * RING + turn(y, dy)) * 2 + (1 - core if other else core)
        return (fs, turn(x, dx))

    barrier = pltpu.get_barrier_semaphore()
    neighbours = [device(other=True)] + [
        device(**{axis: sign}) for axis in ("dz", "dy", "dx") for sign in (1, -1)
    ]
    for neighbour in neighbours:
        pl.semaphore_signal(barrier, inc=1, device_id=neighbour, device_id_type=MESH)

    rows = up_in.shape[0]
    tables = (up_ref, down_ref)

    def weight_rows(unit):
        matrix, order, hz, hy, half = unit
        source = (turn(z, -hz) * RING + turn(y, -hy)) * 2 + core
        start = pl.multiple_of(source * rows + (order * 2 + half) * UNIT, UNIT)
        return tables[matrix].at[pl.ds(start, UNIT), :]

    def weight_copy(index, link, unit):
        ref = weight_rows(unit)
        to = device(**{"d" + link[0]: link[1]})
        return pltpu.make_async_remote_copy(ref, ref, w_send, w_recv.at[index], to, MESH)

    def partner_copy(unit):
        ref = weight_rows(unit)
        return pltpu.make_async_remote_copy(ref, ref, p_send, p_recv.at[unit[0]], device(other=True), MESH)

    def token_copy(index, sign, hops, piece):
        at = pl.ds(piece * PIECE, PIECE)
        there = all_ref.at[turn(x, -sign * hops), at, :]
        here = tok_ref.at[at, :] if hops == 0 else there
        return pltpu.make_async_remote_copy(here, there, t_send, t_recv.at[index], device(dx=sign), MESH)

    w_index = {}
    for leaving in weights:
        for entry in leaving:
            w_index[entry] = len(w_index)
    t_index = {entry: i for i, entry in enumerate(sorted(sum(token_slots[0], [])))}

    def send_weights(slot):
        if slot < len(weights):
            for link, unit in weights[slot]:
                weight_copy(w_index[link, unit], link, unit).start()

    def send_tokens(which, slot):
        if slot < len(token_slots[which]):
            for entry in token_slots[which][slot]:
                token_copy(t_index[entry], *entry).start()

    def receive_weights(slot):
        for link, unit in weights[slot]:
            got = arrived(link, unit)
            ref = weight_rows(got)
            pltpu.make_async_remote_copy(
                ref, ref, w_send, w_recv.at[w_index[link, unit]], device(other=True), MESH
            ).wait_recv()
            partner_copy(got).start()

    def receive_tokens(which, slot):
        for sign, hops, piece in token_slots[which][slot]:
            at = pl.ds(piece * PIECE, PIECE)
            ref = all_ref.at[turn(x, -sign * (hops + 1)), at, :]
            pltpu.make_async_remote_copy(
                ref, ref, t_send, t_recv.at[t_index[sign, hops, piece]], device(other=True), MESH
            ).wait_recv()

    def first_tokens(which):
        for slot in range(TOKEN_LAG):
            send_tokens(which, slot)

    def next_tokens(which, slot):
        receive_tokens(which, slot)
        send_tokens(which, slot + TOKEN_LAG)

    pl.semaphore_wait(barrier, len(neighbours))

    @pl.when(core == 0)
    def _():
        first_tokens(0)

    mine = pl.ds(pl.multiple_of(((z * RING + y) * 2 + core) * rows, rows), rows)
    square = (rows, rows)
    diagonal = lax.broadcasted_iota(jnp.int32, square, 0) == lax.broadcasted_iota(jnp.int32, square, 1)
    for load in loads[:3]:
        load.wait()
    gain = jnp.sum(jnp.where(diagonal, jnp.broadcast_to(gain_ref[...], square), 0.0), axis=1, keepdims=True)
    up_ref[mine, :] = (gain * up_own[...]).astype(BF16)
    down_ref[mine, :] = down_own[...].astype(BF16)
    for slot in range(LAG):
        send_weights(slot)
    for matrix in (0, 1):
        for order in (0, 1):
            for half in (0, 1):
                partner_copy((matrix, order, 0, 0, half)).start()

    def settle(ref, sem):
        pltpu.make_async_copy(ref, ref, sem).wait()

    half_rows = up_ref.shape[0] // 2
    done = [0, 0]

    def advance(which, count):
        count = min(count, len(token_slots[which]) - done[which])
        for slot in range(done[which], done[which] + count):
            next_tokens(which, slot)
        done[which] += count

    for slot in range(len(weights)):
        receive_weights(slot)
        send_weights(slot + LAG)
        for which in (0, 1):

            @pl.when(core == which)
            def _(slot=slot, which=which):
                if which == 1 and slot == TURN:
                    first_tokens(which)
                advance(which, PACE[which][slot])

        if slot == READY:
            loads[3].wait()
            settle(up_ref.at[pl.ds(0, half_rows), :], p_recv.at[0])
        if slot in HIDE[0] and slot in HIDE[1]:
            hide(all_ref, up_ref, hidden_ref, jnp.where(core == 0, HIDE[0][slot], HIDE[1][slot]))
        elif slot in HIDE[0] or slot in HIDE[1]:
            which = 0 if slot in HIDE[0] else 1

            @pl.when(core == which)
            def _(step=HIDE[which][slot]):
                hide(all_ref, up_ref, hidden_ref, step)

    @pl.when(core == 0)
    def _():
        advance(0, len(token_slots[0]))

    @pl.when(core == 1)
    def _():
        for step in range(len(HIDE[1]), hidden_ref.shape[0] // CHUNK):
            last = max(i for i, leaving in enumerate(token_slots[1]) for entry in leaving if entry[2] * PIECE // CHUNK == step)
            advance(1, last + 1 - done[1])
            hide(all_ref, up_ref, hidden_ref, step)
        advance(1, len(token_slots[1]))

    settle(down_ref.at[pl.ds(0, half_rows), :], p_recv.at[1])
    for matrix in (0, 1):
        settle(tables[matrix].at[pl.ds(0, half_rows), :], p_send)
        settle(tables[matrix].at[pl.ds(0, len(w_index) // 2 * UNIT), :], w_send)
    for _ in range(len(t_index) * PIECE // all_ref.shape[1]):
        settle(all_ref.at[0], t_send)


def hide(all_ref, up_ref, hidden_ref, step):
    sources, _, width = all_ref.shape
    features, units = up_ref.shape
    tile = 512
    at = pl.ds(step * CHUNK if isinstance(step, int) else pl.multiple_of(step * CHUNK, CHUNK), CHUNK)
    pieces = [all_ref[k, at, :].astype(F32) for k in range(sources)]
    total = sum(jnp.sum(p * p, axis=-1, keepdims=True) for p in pieces)
    scale = lax.rsqrt(total * (1.0 / features) + epsilon)
    normed = [(p * scale).astype(BF16) for p in pieces]
    for t in range(units // tile):
        cols = pl.ds(t * tile, tile)
        acc = jnp.zeros((CHUNK, tile), F32)
        for k in range(sources):
            acc += jnp.dot(normed[k], up_ref[pl.ds(k * width, width), cols], preferred_element_type=F32)
        hidden_ref[at, cols] = jnp.square(jnp.maximum(acc, 0.0)).astype(BF16)


TARGETS = (2, 1, -1, 0)


def store_kernel(which, up_ref, down_ref, *refs):
    *extra, up_out, down_out = refs[:-1] if len(refs) == 3 else (refs[0], *refs[3:5])
    sem = refs[-1]
    copies = []
    for m, (src, dst) in enumerate(((up_ref, up_out), (down_ref, down_out))):
        part = src.shape[0] // 4
        for i in range(4):
            at = pl.ds(i * part, part)
            copies.append(pltpu.make_async_copy(src.at[at, :], dst.at[at, :], sem.at[m * 4 + i]))

    if extra:
        more = pltpu.make_async_copy(extra[0], refs[5], sem.at[8])
        more.start()

    @pl.when(lax.rem(lax.axis_index("fs"), 2) == which)
    def _():
        for copy in copies:
            copy.start()
        for copy in copies:
            copy.wait()

    if extra:
        more.wait()


def apply_kernel(
    up_ref, down_ref, hidden_ref, stored_ref, out_ref,
    far_ref, right_ref, left_ref, mine_ref, far_left, far_right, from_left, from_right,
    send_sem, far_recv, near_recv,
):
    z, y, core, x = place()
    fs = (z * RING + y) * 2 + core
    right, left = (fs, turn(x, 1)), (fs, turn(x, -1))
    barrier = pltpu.get_barrier_semaphore()
    for neighbour in (right, left):
        pl.semaphore_signal(barrier, inc=1, device_id=neighbour, device_id_type=MESH)

    tokens, width = out_ref.shape
    steps, half = tokens // CHUNK, CHUNK // 2

    def span(step, part=None):
        if part is None:
            return pl.ds(pl.multiple_of(step * CHUNK, CHUNK), CHUNK)
        return pl.ds(pl.multiple_of(step * CHUNK + part * half, half), half)

    def packed(step):
        return pl.ds(pl.multiple_of(step * half, half), half)

    def far_copy(step, part):
        to, dst = (right, far_left) if part == 0 else (left, far_right)
        return pltpu.make_async_remote_copy(
            far_ref.at[span(step, part), :], dst.at[packed(step), :], send_sem, far_recv.at[step, part], to, MESH
        )

    def near_copy(step, side, part):
        to, src, dst = (right, right_ref, from_left) if side == 0 else (left, left_ref, from_right)
        return pltpu.make_async_remote_copy(
            src.at[span(step, part), :], dst.at[span(step, part), :], send_sem, near_recv.at[step, side, part], to, MESH
        )

    def pass_on(step):
        for part, buf, got in ((0, right_ref, far_left), (1, left_ref, far_right)):
            far_copy(step, part).wait_recv()
            at = span(step, part)
            buf[at, :] = (buf[at, :].astype(F32) + got[packed(step), :].astype(F32)).astype(BF16)
            near_copy(step, part, part).start()

    partials = (far_ref, right_ref, left_ref, mine_ref)

    def send_far(step):
        for part in (0, 1):
            far_copy(step, part).start()

    def send_near(step):
        near_copy(step, 0, 1).start()
        near_copy(step, 1, 0).start()

    def multiply(step, first):
        at = span(step)

        def block(by):
            cols = pl.ds(pl.multiple_of(turn(x, by) * width, width), width)
            return lax.dot_general(
                hidden_ref[at, :], down_ref[cols, :], (((1,), (1,)), ((), ())), preferred_element_type=F32
            ).astype(BF16)

        far_ref[at, :] = block(TARGETS[0])
        if first:
            pl.semaphore_wait(barrier, 2)
        send_far(step)
        if not first:
            pass_on(step - 1)
        for buf, by in zip(partials[1:], TARGETS[1:]):
            buf[at, :] = block(by)
        send_near(step)

    multiply(0, True)

    def body(step, carry):
        multiply(step, False)
        return carry

    lax.fori_loop(1, steps, body, 0)
    pass_on(steps - 1)

    def finish(step, carry):
        for part in (0, 1):
            for side in (0, 1):
                near_copy(step, side, part).wait_recv()
        at = span(step)
        total = mine_ref[at, :].astype(F32) + from_left[at, :].astype(F32) + from_right[at, :].astype(F32)
        out_ref[at, :] = total.astype(BF16)
        return carry

    lax.fori_loop(0, steps, finish, 0)
    for buf in (far_ref, right_ref, left_ref):
        pltpu.make_async_copy(buf, buf, send_sem).wait()


def on_device(tokens, norm_gain, up_weight, down_weight):
    count, width = tokens.shape
    features, units = width * RING, up_weight.shape[1]
    weights, token_slots = weight_plan(), [token_plan(count // PIECE, which == 0) for which in (0, 1)]
    steps = count // CHUNK
    vmem, hbm = pl.BlockSpec(memory_space=pltpu.VMEM), pl.BlockSpec(memory_space=pltpu.HBM)
    dma = pltpu.SemaphoreType.DMA
    matrix = (features, units)
    up, down, hidden = pl.pallas_call(
        functools.partial(gather_kernel, weights, token_slots),
        name="gather",
        out_shape=[pltpu.VMEM(matrix, BF16), pltpu.VMEM(matrix, BF16), pltpu.VMEM((count, units), BF16)],
        in_specs=[hbm] * 4,
        out_specs=[vmem] * 3,
        scratch_shapes=[
            pltpu.VMEM((RING, count, width), BF16),
            pltpu.VMEM((1, norm_gain.shape[0]), F32), pltpu.VMEM(up_weight.shape, F32), pltpu.VMEM(up_weight.shape, F32),
            dma((sum(map(len, weights)),)), dma((sum(map(len, token_slots[0])),)), dma, dma, dma, dma((2,)), dma((4,)),
        ],
        compiler_params=pltpu.CompilerParams(collective_id=0, has_side_effects=True, vmem_limit_bytes=33 * 2**20),
    )(tokens, norm_gain[None, :], up_weight, down_weight)
    whole = jax.ShapeDtypeStruct(matrix, BF16)

    def pinned(*arrays):
        return [pltpu.with_memory_space_constraint(a, pltpu.VMEM) for a in arrays]

    stored = pl.pallas_call(
        functools.partial(store_kernel, 1),
        name="store",
        out_shape=[whole, whole],
        in_specs=[vmem] * 2,
        out_specs=[hbm] * 2,
        scratch_shapes=[dma((8,))],
        compiler_params=pltpu.CompilerParams(vmem_limit_bytes=8 * 2**20),
    )(*pinned(up, down))
    rows, half_rows = pltpu.VMEM((count, width), BF16), pltpu.VMEM((count // 2, width), BF16)
    mixed = pl.pallas_call(
        apply_kernel,
        name="apply",
        out_shape=pltpu.VMEM((count, width), BF16),
        in_specs=[vmem] * 3 + [hbm],
        out_specs=vmem,
        scratch_shapes=[
            rows, rows, rows, rows, half_rows, half_rows, rows, rows,
            dma, dma((steps, 2)), dma((steps, 2, 2)),
        ],
        compiler_params=pltpu.CompilerParams(collective_id=1, has_side_effects=True, vmem_limit_bytes=31 * 2**20),
    )(*pinned(up, down, hidden), stored[0])
    return pl.pallas_call(
        functools.partial(store_kernel, 0),
        name="finish",
        out_shape=[whole, whole, jax.ShapeDtypeStruct((count, width), BF16)],
        in_specs=[vmem] * 3 + [hbm] * 2,
        out_specs=[hbm] * 3,
        scratch_shapes=[dma((9,))],
        input_output_aliases={3: 0, 4: 1},
        compiler_params=pltpu.CompilerParams(vmem_limit_bytes=8 * 2**20),
    )(*pinned(up, down, mixed), *stored)


def solution(mesh):
    return jax.shard_map(
        on_device,
        mesh=mesh,
        in_specs=(P("fs", "tp"), P("fs"), P("fs", "tp"), P("fs", "tp")),
        out_specs=(P(None, "tp"), P(None, "tp"), P("fs", "tp")),
        check_vma=False,
    )
```
